32 devices in a mesh: ep: 8 (over z, core), tp: 4 (over y, x).
Axes of the slice: x: 2, y: 2, z: 4, core: 2. Of those that a mesh axis runs over, the one named last changes fastest.
Arguments:
- receptance: bfloat16 [2048, 2048], P('ep', 'tp'), may hold values from -6 to 6
- key_tensor: bfloat16 [2048, 2048], P('ep', 'tp'), may hold values from -6 to 6
- value_tensor: bfloat16 [2048, 2048], P('ep', 'tp'), may hold values from -6 to 6
- decay_data_input: bfloat16 [2048, 2048], P('ep', 'tp'), may hold values from -4 to 4
- correction_rate_input: bfloat16 [2048, 2048], P('ep', 'tp'), may hold values from -16 to 6
- mixer_output_gate: bfloat16 [2048, 2048], P('ep', 'tp'), may hold values from -6 to 6
- decay_channel_offset: float32 [2048], P('tp'), may hold values from -16 to -3
- head_norm_gain: float32 [2048], P('tp'), may hold values from 0.1 to 1.9
- self_key_weight: float32 [2048], P('tp'), may hold values from -2 to 2
- mixer_output_weight: bfloat16 [2048, 2048], P('tp'), may hold values from -0.125 to 0.125
- second_batch_rows: bfloat16 [1024, 2048], P('ep'), may hold values from -6 to 6
- routed_expert_index: int32 [1024, 4], P('ep'), may hold values from 0 to 7, all different within a row; in each aligned block of 128 rows (0 to 127, 128 to 255, ...) at most 96 rows name the same one
- routing_output_weight: float32 [1024, 4], P('ep'), may hold values from 0.1 to 1
- expert_norm_gain: float32 [2048], replicated, may hold values from 0.1 to 1.9
- expert_gate_weight: bfloat16 [8, 1024, 2048], P('ep', 'tp'), may hold values from -0.125 to 0.125
- expert_up_weight: bfloat16 [8, 1024, 2048], P('ep', 'tp'), may hold values from -0.125 to 0.125
- expert_down_weight: bfloat16 [8, 1024, 2048], P('ep', None, 'tp'), may hold values from -0.1875 to 0.1875
- common_expert_gate: bfloat16 [1024, 2048], P('tp'), may hold values from -0.125 to 0.125
- common_expert_up: bfloat16 [1024, 2048], P('tp'), may hold values from -0.125 to 0.125
- common_expert_down: bfloat16 [1024, 2048], P(None, 'tp'), may hold values from -0.1875 to 0.1875
Outputs:
- token_mixer_output: bfloat16 [2048, 2048], P(('ep', 'tp'))
- expert_out: bfloat16 [1024, 2048], P('ep', 'tp')
The draws below stay inside these ranges and needn't reach their ends.
Inputs may be any that keep to these rules, and one draw needn't show every extreme that they name: `routed_expert_index`: each row names 4 different experts. Within the rows of one index of ep no expert is named by more than 96 rows, and that bound is met in some index's rows.
All inputs are finite; a program needn't handle non-finite values.
Results may differ from the reference program's by a relative error of at most 0.017.
Values may be sent and summed in bfloat16 or wider, within the bound.
A program may use at most 128 MiB of HBM per device.

```python
import math
import jax
import jax.numpy as jnp
import numpy as np
from jax import lax

MODEL_WIDTH = 2048
HEADS = 32
HEAD_CHANNELS = 64
FF = 1024
TOP = 4
ROWS_EXP = 128
SEQ_MIX = 2048
TOKENS_EXP = 1024
EXPERTS = 8
CAP = 96
N_EP = 8
N_TP = 4


def slow_marks(key):
    picks = jax.random.randint(jax.random.fold_in(key, 7), (HEADS,), 0, 10)
    return picks < 5


def draw_decay_channel_offset(key, part):
    slow_heads = slow_marks(key)
    spread = jax.random.uniform(jax.random.fold_in(key, 11), (HEADS, HEAD_CHANNELS), jnp.float32)
    slow_base = jnp.log(0.4 / SEQ_MIX) + 0.5 - spread
    fast_base = -4.0 + spread
    return jnp.where(slow_heads[:, None], slow_base, fast_base).reshape(MODEL_WIDTH).astype(jnp.float32)


def draw_correction_rate_input(key, part):
    slow_heads = slow_marks(key)
    offset = jnp.where(slow_heads, jnp.log(0.3 * HEAD_CHANNELS / SEQ_MIX), 0.0)
    jitter = jnp.clip(jax.random.normal(jax.random.fold_in(key, 13), (SEQ_MIX, HEADS, HEAD_CHANNELS), jnp.float32), -6.0, 6.0)
    return (jitter + offset[None, :, None]).reshape(SEQ_MIX, MODEL_WIDTH).astype(jnp.bfloat16)


def draw_decay_data_input(key, part):
    blocks = SEQ_MIX // 64
    shifts = jax.random.uniform(jax.random.fold_in(key, 17), (blocks, 1, MODEL_WIDTH), jnp.float32, -1.0, 1.0)
    jitter = 0.6 * jnp.clip(jax.random.normal(jax.random.fold_in(key, 19), (blocks, 64, MODEL_WIDTH), jnp.float32), -5.0, 5.0)
    return (jitter + shifts).reshape(SEQ_MIX, MODEL_WIDTH).astype(jnp.bfloat16)


def level_of(own_key, shape, shards, least, top_value):
    loudness, own = 1.0, jax.random.fold_in(own_key, 6)
    for axis_at, blocks in shards:
        draws = jnp.exp(jax.random.uniform(jax.random.fold_in(own, axis_at), (blocks,), jnp.float32, least / len(shards), top_value / len(shards)))
        loudness = loudness * jnp.repeat(draws, shape[axis_at] // blocks).reshape([-1 if axis == axis_at else 1 for axis in range(len(shape))])
    return loudness


def deal_out(own_key, own, number, rows, count, top, reach, slope):
    order = jax.random.permutation(own_key, count)
    crowded, ordinary = portions_of(count, rows * top, reach, slope, True), portions_of(count, rows * top, reach, slope, False)
    places = jnp.arange(count)

    def named(lengths, rotation):
        used = int((lengths > 0).sum())
        fixed = max(1, used // 4)
        moved = fixed + (places - fixed + rotation * (used - fixed)) % max(1, count - fixed)
        return jnp.zeros((count,), jnp.int32).at[order[jnp.where(places < fixed, places, moved)]].set(jnp.asarray(lengths, jnp.int32))

    lengths = jnp.where(number % 4 == 0, named(crowded, number // 4), named(ordinary, number - number // 4 - 1))
    mixed = jax.random.permutation(jax.random.fold_in(own, 3), count)
    source_of, taker = mixed[0:count // 2 * 2:2], mixed[1:count // 2 * 2:2]
    slack = jnp.minimum(lengths[source_of] - 1, reach - lengths[taker]) // 2
    slack = jnp.where((source_of == order[0]) | (taker == order[0]) | (lengths[taker] == 0), 0, jnp.maximum(slack, 0))
    moved = jax.random.randint(jax.random.fold_in(own, 4), (count // 2,), 0, 1 << 20) % (slack + 1)
    lengths = lengths.at[source_of].add(-moved).at[taker].add(moved)
    labels = jnp.searchsorted(jnp.cumsum(lengths), jnp.arange(rows * top), side="right").astype(jnp.int32)
    grid = labels.reshape(top, rows).T
    grid = grid[jax.random.permutation(jax.random.fold_in(own, 1), rows)]
    rotation = jax.random.randint(jax.random.fold_in(own, 2), (rows, 1), 0, top)
    return jnp.take_along_axis(grid, (jnp.arange(top)[None, :] + rotation) % top, axis=1)


def portions_of(amount, total, bound, skew, full):
    loads = [(1 << 20) // math.isqrt(grade ** skew) + 1 for grade in range(1, amount + 1)]
    largest = bound if full else min(bound, max(-(-total // amount), total * loads[0] // sum(loads)))
    least = 1 if total - largest >= amount - 1 else 0
    given, rest = [largest] + [least] * (amount - 1), total - largest - least * (amount - 1)
    while rest > 0:
        candidates = [i for i in range(1, amount) if given[i] < largest] or [i for i in range(1, amount) if given[i] < bound]
        whole, budget = sum([loads[i] for i in candidates]), rest
        for i in candidates:
            extra = min(bound - given[i], max(1, budget * loads[i] // whole), rest)
            given[i] = given[i] + extra
            rest = rest - extra
    return np.array(given)


def noise(own_key, extent, deviation, bound, cuts=(), kind=jnp.bfloat16):
    gain = level_of(own_key, extent, cuts, -0.22, 0.18) if cuts else 1.0
    values = jax.random.normal(own_key, extent, jnp.float32) * deviation * gain
    return jnp.minimum(jnp.maximum(values, -bound), bound).astype(kind)


def setup_inputs(seed: int = 0) -> dict:
    keys = jax.random.split(jax.random.key(seed), 21)
    receptance = noise(keys[0], (SEQ_MIX, MODEL_WIDTH), 1.0, 6.0, ((0, 8), (1, 4)))
    key_tensor = noise(keys[1], (SEQ_MIX, MODEL_WIDTH), 1.0, 6.0, ((0, 8), (1, 4)))
    value_tensor = noise(keys[2], (SEQ_MIX, MODEL_WIDTH), 1.0, 6.0, ((0, 8), (1, 4)))
    decay_data_input = draw_decay_data_input(jax.random.fold_in(keys[20], 71), 0)
    correction_rate_input = draw_correction_rate_input(jax.random.fold_in(keys[20], 71), 0)
    mixer_output_gate = noise(keys[5], (SEQ_MIX, MODEL_WIDTH), 1.0, 6.0, ((0, 8), (1, 4)))
    decay_channel_offset = draw_decay_channel_offset(jax.random.fold_in(keys[20], 71), 0)
    head_norm_gain = jnp.clip(1.0 + 0.18 * jax.random.normal(keys[7], (MODEL_WIDTH,), jnp.float32), 0.1, 1.9)
    self_key_weight = noise(keys[8], (MODEL_WIDTH,), 0.15, 2.0, ((0, 4),), jnp.float32)
    mixer_output_weight = noise(keys[9], (MODEL_WIDTH, MODEL_WIDTH), MODEL_WIDTH ** -0.5, 0.125, ((0, 4),))
    second_batch_rows = noise(keys[10], (TOKENS_EXP, MODEL_WIDTH), 1.0, 6.0, ((0, 8),))
    routed_expert_index_keys = jax.random.split(jax.random.fold_in(keys[11], 1), TOKENS_EXP // ROWS_EXP)
    routed_expert_index_turns = jax.random.permutation(jax.random.fold_in(keys[11], 3), TOKENS_EXP // ROWS_EXP)
    routed_expert_index = jax.vmap(lambda own, number: deal_out(jax.random.fold_in(keys[11], 2), own, number, ROWS_EXP, EXPERTS, TOP, CAP, 1))(routed_expert_index_keys, routed_expert_index_turns).reshape((TOKENS_EXP, TOP))
    routing_output_weight = jnp.clip(0.1 + 0.9 * jax.random.uniform(keys[12], (TOKENS_EXP, TOP), jnp.float32) ** level_of(keys[12], (TOKENS_EXP, TOP), ((0, 8),), -0.2, 0.2), 0.1, 1.0)
    expert_norm_gain = jnp.clip(1.0 + 0.18 * jax.random.normal(keys[13], (MODEL_WIDTH,), jnp.float32), 0.1, 1.9)
    expert_gate_weight = noise(keys[14], (EXPERTS, FF, MODEL_WIDTH), MODEL_WIDTH ** -0.5, 0.125, ((0, 8), (1, 4)))
    expert_up_weight = noise(keys[15], (EXPERTS, FF, MODEL_WIDTH), MODEL_WIDTH ** -0.5, 0.125, ((0, 8), (1, 4)))
    expert_down_weight = noise(keys[16], (EXPERTS, FF, MODEL_WIDTH), FF ** -0.5, 0.1875, ((0, 8), (2, 4)))
    common_expert_gate = noise(keys[17], (FF, MODEL_WIDTH), MODEL_WIDTH ** -0.5, 0.125, ((0, 4),))
    common_expert_up = noise(keys[18], (FF, MODEL_WIDTH), MODEL_WIDTH ** -0.5, 0.125, ((0, 4),))
    common_expert_down = noise(keys[19], (FF, MODEL_WIDTH), FF ** -0.5, 0.1875, ((1, 4),))
    return dict(receptance=receptance, key_tensor=key_tensor, value_tensor=value_tensor, decay_data_input=decay_data_input, correction_rate_input=correction_rate_input, mixer_output_gate=mixer_output_gate, decay_channel_offset=decay_channel_offset, head_norm_gain=head_norm_gain, self_key_weight=self_key_weight, mixer_output_weight=mixer_output_weight, second_batch_rows=second_batch_rows, routed_expert_index=routed_expert_index, routing_output_weight=routing_output_weight, expert_norm_gain=expert_norm_gain, expert_gate_weight=expert_gate_weight, expert_up_weight=expert_up_weight, expert_down_weight=expert_down_weight, common_expert_gate=common_expert_gate, common_expert_up=common_expert_up, common_expert_down=common_expert_down)


HIGHEST = lax.Precision.HIGHEST
NORM_FLOOR = 1.0

def decay_terms(decay_data_input, correction_rate_input, decay_channel_offset):
    pre_log = -jax.nn.softplus(-(decay_channel_offset + decay_data_input.astype(jnp.float32))) - 0.5
    return (jnp.exp(-jnp.exp(pre_log)), jax.nn.sigmoid(correction_rate_input.astype(jnp.float32)))

def head_view(matrix):
    return matrix.astype(jnp.float32).reshape(matrix.shape[0], -1, HEAD_CHANNELS)

def complete_head_outputs(state_readout, receptance_rows, key_row_block, value_row_block, head_norm_gain, self_key_weight, mixer_output_gate):
    mean_part = lax.optimization_barrier(jnp.mean(state_readout, axis=-1, keepdims=True))
    spread = lax.optimization_barrier(jnp.mean(jnp.square(state_readout - mean_part), axis=-1, keepdims=True))
    normalized_rows = (state_readout - mean_part) * lax.rsqrt(spread + NORM_FLOOR)
    sequence_length = state_readout.shape[0]
    normalized_rows = normalized_rows.reshape(sequence_length, -1) * head_norm_gain
    self_key_term = lax.optimization_barrier(jnp.sum(receptance_rows * key_row_block * self_key_weight.reshape(-1, HEAD_CHANNELS), axis=-1, keepdims=True)) * value_row_block
    mixer_result = (normalized_rows + self_key_term.reshape(sequence_length, -1)) * mixer_output_gate.astype(jnp.float32)
    return mixer_result.astype(jnp.bfloat16)

def token_mixer_baseline(receptance, key_tensor, value_tensor, decay_data_input, correction_rate_input, mixer_output_gate, decay_channel_offset, head_norm_gain, self_key_weight, mixer_output_weight):
    decays, rates = decay_terms(decay_data_input, correction_rate_input, decay_channel_offset)
    receptance_rows = head_view(receptance)
    key_row_block = head_view(key_tensor)
    value_row_block = head_view(value_tensor)
    unit_keys = key_row_block * lax.rsqrt(lax.optimization_barrier(jnp.sum(key_row_block * key_row_block, axis=-1, keepdims=True)) + 1.0)
    decays = decays.reshape(key_row_block.shape)
    rates = rates.reshape(key_row_block.shape)

    def advance(memory, inputs):
        recept_now, decay_now, key_now, value_now, unit_now, rate_now = inputs
        projected = jnp.einsum('hij,hj->hi', memory, unit_now, precision=HIGHEST)
        memory = memory * decay_now[:, None, :] - projected[:, :, None] * (unit_now * rate_now)[:, None, :] + value_now[:, :, None] * key_now[:, None, :]
        return (memory, jnp.einsum('hij,hj->hi', memory, recept_now, precision=HIGHEST))
    head_count = key_row_block.shape[1]
    initial = jnp.zeros((head_count, HEAD_CHANNELS, HEAD_CHANNELS), jnp.float32)
    _, state_readout = lax.scan(advance, initial, (receptance_rows, decays, key_row_block, value_row_block, unit_keys, rates))
    mixer_result = complete_head_outputs(state_readout, receptance_rows, key_row_block, value_row_block, head_norm_gain, self_key_weight, mixer_output_gate)
    groups = mixer_result.reshape(SEQ_MIX, N_TP, MODEL_WIDTH // N_TP).transpose(1, 0, 2)
    weights = mixer_output_weight.reshape(N_TP, MODEL_WIDTH // N_TP, MODEL_WIDTH)

    def add_group(running, blocks):
        mixed_part, weight_part = blocks
        partial_sum = jnp.dot(mixed_part, weight_part, preferred_element_type=jnp.float32).astype(jnp.bfloat16)
        partial_sum = lax.optimization_barrier(partial_sum)
        return (running + partial_sum.astype(jnp.float32), None)
    summed, _ = lax.scan(add_group, jnp.zeros((SEQ_MIX, MODEL_WIDTH), jnp.float32), (groups, weights))
    return summed.astype(jnp.bfloat16)

def expert_unit(rows_in, gate_part, up_part, down_part):
    pre_gate = jnp.dot(rows_in, gate_part.T, preferred_element_type=jnp.float32)
    pre_up = jnp.dot(rows_in, up_part.T, preferred_element_type=jnp.float32)
    hidden = (jax.nn.silu(pre_gate) * pre_up).astype(jnp.bfloat16)
    return jnp.dot(hidden, down_part, preferred_element_type=jnp.float32)

def experts_reference(second_batch_rows, routed_expert_index, routing_output_weight, expert_norm_gain, expert_gate_weight, expert_up_weight, expert_down_weight, common_expert_gate, common_expert_up, common_expert_down):
    widened = second_batch_rows.astype(jnp.float32)
    normalized_rows = (widened * lax.rsqrt(lax.optimization_barrier(jnp.mean(widened * widened, axis=-1, keepdims=True)) + NORM_FLOOR) * expert_norm_gain).astype(jnp.bfloat16)
    shared_out = expert_unit(normalized_rows, common_expert_gate, common_expert_up, common_expert_down)
    flat_ids = routed_expert_index.reshape(-1).astype(jnp.int32)
    ordering = jnp.argsort(flat_ids, stable=True).astype(jnp.int32)
    counts = lax.optimization_barrier(jnp.sum((flat_ids[:, None] == jnp.arange(EXPERTS, dtype=jnp.int32)[None, :]).astype(jnp.int32), axis=0))
    firsts = (jnp.cumsum(counts) - counts).astype(jnp.int32)
    capacity = N_EP * CAP
    padded_order = jnp.concatenate([ordering, jnp.zeros((capacity,), jnp.int32)])
    flat_weights = routing_output_weight.reshape(-1)

    def visit(summed, expert):
        chosen = lax.dynamic_slice_in_dim(padded_order, firsts[expert], capacity)
        usable = jnp.arange(capacity) < counts[expert]
        tokens = chosen // TOP
        copies = expert_unit(normalized_rows[tokens], expert_gate_weight[expert], expert_up_weight[expert], expert_down_weight[expert]).astype(jnp.bfloat16)
        copies = lax.optimization_barrier(copies).astype(jnp.float32)
        factor = jnp.where(usable, flat_weights[chosen], 0.0)
        return (summed.at[tokens].add(copies * factor[:, None]), None)
    routed, _ = lax.scan(visit, jnp.zeros((TOKENS_EXP, MODEL_WIDTH), jnp.float32), jnp.arange(EXPERTS))
    return (routed + shared_out).astype(jnp.bfloat16)

def reference(receptance, key_tensor, value_tensor, decay_data_input, correction_rate_input, mixer_output_gate, decay_channel_offset, head_norm_gain, self_key_weight, mixer_output_weight, second_batch_rows, routed_expert_index, routing_output_weight, expert_norm_gain, expert_gate_weight, expert_up_weight, expert_down_weight, common_expert_gate, common_expert_up, common_expert_down):
    token_mixer_output = token_mixer_baseline(receptance, key_tensor, value_tensor, decay_data_input, correction_rate_input, mixer_output_gate, decay_channel_offset, head_norm_gain, self_key_weight, mixer_output_weight)
    expert_out = experts_reference(second_batch_rows, routed_expert_index, routing_output_weight, expert_norm_gain, expert_gate_weight, expert_up_weight, expert_down_weight, common_expert_gate, common_expert_up, common_expert_down)
    return (token_mixer_output, expert_out)
```

```python
import math

import jax
import jax.numpy as jnp
from jax import lax
from jax.sharding import PartitionSpec as P

HEAD_CHANNELS = 64
SPAN = 64
HIGHEST = lax.Precision.HIGHEST
PRECISION = lax.Precision.HIGH
NORM_FLOOR = 1.0


def head_view(matrix):
    return matrix.astype(jnp.float32).reshape(matrix.shape[0], -1, HEAD_CHANNELS)


def complete_head_outputs(
    state_readout,
    receptance_rows,
    key_row_block,
    value_row_block,
    head_norm_gain,
    self_key_weight,
    mixer_output_gate,
):
    mean_part = jnp.mean(state_readout, axis=-1, keepdims=True)
    spread = jnp.mean(jnp.square(state_readout - mean_part), axis=-1, keepdims=True)
    normalized_rows = (state_readout - mean_part) * lax.rsqrt(spread + NORM_FLOOR)
    sequence_length = state_readout.shape[0]
    normalized_rows = normalized_rows.reshape(sequence_length, -1) * head_norm_gain
    self_key_term = (
        jnp.sum(
            receptance_rows * key_row_block * self_key_weight.reshape(-1, HEAD_CHANNELS),
            axis=-1,
            keepdims=True,
        )
        * value_row_block
    )
    mixer_result = (
        normalized_rows + self_key_term.reshape(sequence_length, -1)
    ) * mixer_output_gate.astype(jnp.float32)
    return mixer_result.astype(jnp.bfloat16)


def product(spec, left, right):
    return jnp.einsum(spec, left, right, precision=PRECISION, preferred_element_type=jnp.float32)


def lower_inverse(strict, size):
    at = jnp.arange(size)
    row, column = at[:, None], at[None, :]
    inverse = None
    block = 1
    while block < size:
        pair = (
            (row // (2 * block) == column // (2 * block))
            & (row // block % 2 == 1)
            & (column // block % 2 == 0)
        )
        below = jnp.where(pair, strict, 0.0)
        if inverse is None:
            inverse = jnp.eye(size, dtype=jnp.float32) - below
        else:
            inverse = inverse - product(
                "nhij,nhjk->nhik", product("nhij,nhjk->nhik", inverse, below), inverse
            )
        block *= 2
    return inverse


def mixer_part(
    receptance,
    key_tensor,
    value_tensor,
    decay_data_input,
    correction_rate_input,
    mixer_output_gate,
    decay_channel_offset,
    head_norm_gain,
    self_key_weight,
    mixer_output_weight,
):
    row_count, width = receptance.shape
    head_count = width // HEAD_CHANNELS
    span = min(SPAN, row_count)
    block_count = row_count // span
    receptance_rows = head_view(receptance)
    key_row_block = head_view(key_tensor)
    value_row_block = head_view(value_tensor)

    def by_block(matrix):
        return (
            matrix.astype(jnp.float32)
            .reshape(block_count, span, head_count, HEAD_CHANNELS)
            .transpose(0, 2, 1, 3)
        )

    step_log = -math.exp(-0.5) * jax.nn.sigmoid(
        decay_channel_offset + decay_data_input.astype(jnp.float32)
    )
    at = jnp.arange(span)
    reach = (at[:, None] >= at[None, :]).astype(jnp.float32)
    step_log = by_block(step_log)
    total_log = jnp.einsum("ts,nhsd->nhtd", reach, step_log, precision=HIGHEST)
    recept, keys, values = by_block(receptance), by_block(key_tensor), by_block(value_tensor)
    units = keys * lax.rsqrt(jnp.sum(keys * keys, axis=-1, keepdims=True) + 1.0)
    corrections = units * jax.nn.sigmoid(by_block(correction_rate_input))
    grown = jnp.exp(-total_log)
    last_log = total_log[:, :, -1:, :]
    unit_in = units * jnp.exp(total_log - step_log)
    recept_in = recept * jnp.exp(total_log)
    tail = jnp.exp(last_log - total_log)
    scores = product(
        "nhtd,nhsd->nhts",
        jnp.concatenate([unit_in, recept_in], axis=2),
        jnp.concatenate([keys * grown, corrections * grown], axis=2),
    )
    before = at[:, None] > at[None, :]
    upto = at[:, None] >= at[None, :]
    unit_key = jnp.where(before, scores[:, :, :span, :span], 0.0)
    unit_fix = jnp.where(before, scores[:, :, :span, span:], 0.0)
    read_key = jnp.where(upto, scores[:, :, span:, :span], 0.0)
    read_fix = jnp.where(upto, scores[:, :, span:, span:], 0.0)
    inverse = lower_inverse(unit_fix, span)
    key_values = product(
        "nhts,nhsd->nhtd", jnp.concatenate([unit_key, read_key], axis=2), values
    )
    solved = product(
        "nhts,nhsd->nhtd",
        inverse,
        jnp.concatenate([unit_in, key_values[:, :, :span]], axis=3),
    )
    reads = jnp.concatenate([recept_in, key_values[:, :, span:]], axis=3) - product(
        "nhts,nhsd->nhtd", read_fix, solved
    )
    eye_head = jnp.eye(HEAD_CHANNELS, dtype=jnp.float32)
    fresh = product("nhtj,nhti->nhji", keys * tail, values)
    moves = jnp.concatenate(
        [eye_head * jnp.exp(last_log), fresh], axis=3
    ) - product("nhtj,nhti->nhji", corrections * tail, solved)
    whole = moves[0]
    for block in range(1, block_count):
        step = product("hij,hjk->hik", moves[block, :, :, :HEAD_CHANNELS], whole)
        whole = step + jnp.concatenate(
            [jnp.zeros_like(step[..., :HEAD_CHANNELS]), moves[block, :, :, HEAD_CHANNELS:]],
            axis=2,
        )
    everything = lax.all_gather(whole.astype(jnp.bfloat16), "ep")
    mine = lax.axis_index("ep")
    state = jnp.zeros((head_count, HEAD_CHANNELS, HEAD_CHANNELS), jnp.float32)
    for k in range(lax.axis_size("ep") - 1):
        part = everything[k].astype(jnp.float32)
        new = product("hij,hjk->hik", part[..., :HEAD_CHANNELS], state)
        state = jnp.where(k < mine, new + part[..., HEAD_CHANNELS:], state)
    starts = [state]
    for block in range(block_count - 1):
        state = (
            product("hij,hjk->hik", moves[block, :, :, :HEAD_CHANNELS], state)
            + moves[block, :, :, HEAD_CHANNELS:]
        )
        starts.append(state)
    merged_output = reads[..., HEAD_CHANNELS:] + product(
        "nhtj,nhji->nhti", reads[..., :HEAD_CHANNELS], jnp.stack(starts)
    )
    merged_output = merged_output.transpose(0, 2, 1, 3).reshape(
        row_count, head_count, HEAD_CHANNELS
    )
    mixer_result = complete_head_outputs(
        merged_output,
        receptance_rows,
        key_row_block,
        value_row_block,
        head_norm_gain,
        self_key_weight,
        mixer_output_gate,
    )
    return lax.psum_scatter(
        jnp.dot(mixer_result, mixer_output_weight, preferred_element_type=jnp.float32).astype(
            jnp.bfloat16
        ),
        "tp",
        scatter_dimension=0,
        tiled=True,
    )


def activate(rows_in, gate_part, up_part):
    pre_gate = jnp.einsum("fd,rd->fr", gate_part, rows_in, preferred_element_type=jnp.float32)
    pre_up = jnp.einsum("fd,rd->fr", up_part, rows_in, preferred_element_type=jnp.float32)
    return (jax.nn.silu(pre_gate) * pre_up).astype(jnp.bfloat16)


def expert_entry(
    second_batch_rows,
    routed_expert_index,
    routing_output_weight,
    expert_norm_gain,
    common_expert_gate,
    common_expert_up,
):
    row_count, width = second_batch_rows.shape
    top_count = routed_expert_index.shape[1]
    peer_count = lax.axis_size("ep")
    slot_count = 3 * row_count * top_count // (2 * peer_count)
    widened = second_batch_rows.astype(jnp.float32)
    normalized_rows = (
        widened
        * lax.rsqrt(jnp.mean(widened * widened, axis=-1, keepdims=True) + NORM_FLOOR)
        * expert_norm_gain
    ).astype(jnp.bfloat16)
    flat_ids = routed_expert_index.reshape(-1)
    one_hot = (flat_ids[:, None] == jnp.arange(peer_count, dtype=jnp.int32)[None, :]).astype(
        jnp.int32
    )
    slot_rank = jnp.sum((jnp.cumsum(one_hot, axis=0) - 1) * one_hot, axis=1)
    target = flat_ids * slot_count + slot_rank
    owners = jnp.arange(row_count * top_count, dtype=jnp.int32) // top_count
    source_row = jnp.full((peer_count * slot_count,), row_count, jnp.int32).at[target].set(owners)
    padded = jnp.concatenate([normalized_rows, jnp.zeros((1, width), jnp.bfloat16)], axis=0)
    outgoing = jnp.take(padded, source_row, axis=0).reshape(peer_count, slot_count, width)
    shared_hidden = activate(normalized_rows, common_expert_gate, common_expert_up)
    piece_width = width // lax.axis_size("tp")
    own_slice = lax.dynamic_slice_in_dim(
        outgoing, lax.axis_index("tp") * piece_width, piece_width, 2
    )
    arrived = lax.all_to_all(own_slice, "ep", split_axis=0, concat_axis=0, tiled=True)
    return (arrived, shared_hidden, target)


def expert_exit(
    arrived,
    shared_hidden,
    target,
    routing_output_weight,
    expert_gate_weight,
    expert_up_weight,
    expert_down_weight,
    common_expert_down,
):
    peer_count, slot_count, piece_width = arrived.shape
    row_count, top_count = routing_output_weight.shape
    out_width = expert_down_weight.shape[2]
    flat_rows = arrived.reshape(-1, piece_width)
    pieces = lax.all_gather(flat_rows, "tp", axis=1, tiled=True)
    gate_cols = expert_gate_weight[0]
    up_cols = expert_up_weight[0]
    pre_gate = jnp.einsum("fd,rd->fr", gate_cols, pieces, preferred_element_type=jnp.float32)
    pre_up = jnp.einsum("fd,rd->fr", up_cols, pieces, preferred_element_type=jnp.float32)
    routed_hidden = (jax.nn.silu(pre_gate) * pre_up).astype(jnp.bfloat16)
    both = lax.all_gather(
        jnp.concatenate([routed_hidden, shared_hidden], axis=1), "tp", axis=0, tiled=True
    )
    pieces = (both[:, : routed_hidden.shape[1]], both[:, routed_hidden.shape[1] :])
    routed_rows = expert_down_weight[0]
    routed_sum = jnp.einsum("fr,fd->rd", pieces[0], routed_rows, preferred_element_type=jnp.float32)
    shared_out = jnp.einsum(
        "fr,fd->rd", pieces[1], common_expert_down, preferred_element_type=jnp.float32
    )
    returned = lax.all_to_all(
        routed_sum.astype(jnp.bfloat16).reshape(peer_count, slot_count, out_width),
        "ep",
        split_axis=0,
        concat_axis=0,
        tiled=True,
    )
    picked = jnp.take(returned.reshape(-1, out_width), target, axis=0).reshape(
        row_count, top_count, out_width
    )
    merged_output = (
        jnp.sum(picked.astype(jnp.float32) * routing_output_weight[:, :, None], axis=1) + shared_out
    )
    return merged_output.astype(jnp.bfloat16)


def on_device(
    receptance,
    key_tensor,
    value_tensor,
    decay_data_input,
    correction_rate_input,
    mixer_output_gate,
    decay_channel_offset,
    head_norm_gain,
    self_key_weight,
    mixer_output_weight,
    second_batch_rows,
    routed_expert_index,
    routing_output_weight,
    expert_norm_gain,
    expert_gate_weight,
    expert_up_weight,
    expert_down_weight,
    common_expert_gate,
    common_expert_up,
    common_expert_down,
):
    arrived, shared_hidden, target = expert_entry(
        second_batch_rows,
        routed_expert_index,
        routing_output_weight,
        expert_norm_gain,
        common_expert_gate,
        common_expert_up,
    )
    arrived, receptance, key_tensor, value_tensor, decay_data_input, correction_rate_input = (
        lax.optimization_barrier(
            (
                arrived,
                receptance,
                key_tensor,
                value_tensor,
                decay_data_input,
                correction_rate_input,
            )
        )
    )
    token_mixer_output = mixer_part(
        receptance,
        key_tensor,
        value_tensor,
        decay_data_input,
        correction_rate_input,
        mixer_output_gate,
        decay_channel_offset,
        head_norm_gain,
        self_key_weight,
        mixer_output_weight,
    )
    expert_out = expert_exit(
        arrived,
        shared_hidden,
        target,
        routing_output_weight,
        expert_gate_weight,
        expert_up_weight,
        expert_down_weight,
        common_expert_down,
    )
    return (token_mixer_output, expert_out)


def solution(mesh):
    in_specs = (
        P("ep", "tp"),
        P("ep", "tp"),
        P("ep", "tp"),
        P("ep", "tp"),
        P("ep", "tp"),
        P("ep", "tp"),
        P("tp"),
        P("tp"),
        P("tp"),
        P("tp", None),
        P("ep", None),
        P("ep", None),
        P("ep", None),
        P(),
        P("ep", "tp", None),
        P("ep", "tp", None),
        P("ep", None, "tp"),
        P("tp", None),
        P("tp", None),
        P(None, "tp"),
    )
    out_specs = (P(("ep", "tp"), None), P("ep", "tp"))
    return jax.shard_map(
        on_device, mesh=mesh, in_specs=in_specs, out_specs=out_specs, check_vma=False
    )
```
